256 devices in a mesh: rep: 2 (over z_hi), fs: 16 (over z_lo, y), tp: 8 (over x, core).
Axes of the slice: x: 4, y: 4, z: 8 (z_hi: 2, z_lo: 4; z = z_hi * 4 + z_lo), core: 2. Of those that a mesh axis runs over, the one named last changes fastest.
Arguments:
- residual: bfloat16 [32, 384, 2048], P(('rep', 'fs'), None, 'tp'), may hold values from -6 to 6
- gain_first: float32 [2048], replicated, may hold values from 0.1 to 1.9
- gain_mixer: float32 [2048], replicated, may hold values from 0.1 to 1.9
- gain_last: float32 [2048], replicated, may hold values from 0.1 to 1.9
- hidden_gate: float32 [2048, 6144], P('fs', 'tp'), may hold values from -0.125 to 0.125
- hidden_up: float32 [2048, 6144], P('fs', 'tp'), may hold values from -0.125 to 0.125
- hidden_down: float32 [6144, 2048], P('tp', 'fs'), may hold values from -0.078125 to 0.078125
- gate_scale: float32 [6144], replicated, may hold values from 0.5 to 2
- up_scale: float32 [6144], replicated, may hold values from 0.5 to 2
- down_scale: float32 [2048], replicated, may hold values from 0.5 to 2
- mix_value: float32 [2048, 2048], P('fs', 'tp'), may hold values from -0.125 to 0.125
- mix_gate: float32 [2048, 2048], P('fs', 'tp'), may hold values from -0.125 to 0.125
- value_scale: float32 [2048], replicated, may hold values from 0.5 to 2
- gating_scale: float32 [2048], replicated, may hold values from 0.5 to 2
- mix_taps: float32 [31, 2048], replicated, may hold values from -1.25 to 1.25
- mix_gain: float32 [2048], replicated, may hold values from 0.1 to 1.9
- mix_out: float32 [2048, 2048], P('tp', 'fs'), may hold values from -0.125 to 0.125
- out_scale: float32 [2048], replicated, may hold values from 0.5 to 2
Outputs:
- updated: bfloat16 [32, 384, 2048], P(('rep', 'fs'), None, 'tp')
The draws below stay inside these ranges and needn't reach their ends.
All inputs are finite; a program needn't handle non-finite values.
Results may differ from the reference program's by a relative error of at most 0.024.
Values may be sent and summed in bfloat16 or wider, within the bound.
No kernel may reach another device: no remote copies, remote signals or barrier semaphores. Data moves between devices by JAX's collectives and lax.ppermute only.
A program may use at most 64 MiB of HBM per device.

```python
import math
import jax
import jax.numpy as jnp
from jax import lax

D = 2048
FF = 6144
KW = 31
SEQ = 384
SEQS = 32
N_TP = 8


def draw_mix_taps(key, part):
    channel = jnp.arange(D).astype(jnp.float32) / max(D - 1, 1)
    base = jnp.clip(jax.random.normal(key, (KW, D), jnp.float32), -4.0, 4.0)
    ramp = jnp.power(3.0, channel) / jnp.sqrt(3.0)
    return (base * ramp[None, :] * KW ** (-0.5)).astype(jnp.float32)


def steps_of(key, shape, cuts, least, top_value):
    def one(dim, blocks):
        draws = jax.random.uniform(jax.random.fold_in(jax.random.fold_in(key, 6), dim), (blocks,), jnp.float32, least / len(cuts), top_value / len(cuts))
        return jnp.repeat(jnp.exp(draws), shape[dim] // blocks).reshape((-1,) + (1,) * (len(shape) - dim - 1))

    factor_of = one(*cuts[0])
    for cut in cuts[1:]:
        factor_of = factor_of * one(*cut)
    return factor_of


def gaussian(stream_key, shape, deviation, limit, cuts=(), kind=jnp.bfloat16):
    loudness = steps_of(stream_key, shape, cuts, -0.22, 0.18) if cuts else 1.0
    array = jax.random.normal(stream_key, shape, jnp.float32) * deviation * loudness
    return jnp.minimum(jnp.maximum(array, -limit), limit).astype(kind)


def setup_inputs(seed: int = 0) -> dict:
    streams_of = jax.random.split(jax.random.key(seed), 19)
    residual = gaussian(streams_of[0], (SEQS, SEQ, D), 1.0, 6.0, ((0, 32), (2, 8)))
    gain_first = jnp.clip(1.0 + 0.18 * jax.random.normal(streams_of[1], (D,), jnp.float32), 0.1, 1.9)
    gain_mixer = jnp.clip(1.0 + 0.18 * jax.random.normal(streams_of[2], (D,), jnp.float32), 0.1, 1.9)
    gain_last = jnp.clip(1.0 + 0.18 * jax.random.normal(streams_of[3], (D,), jnp.float32), 0.1, 1.9)
    hidden_gate = gaussian(streams_of[4], (D, FF), D ** -0.5, 0.125, ((0, 16), (1, 8)), jnp.float32)
    hidden_up = gaussian(streams_of[5], (D, FF), D ** -0.5, 0.125, ((0, 16), (1, 8)), jnp.float32)
    hidden_down = gaussian(streams_of[6], (FF, D), FF ** -0.5, 0.078125, ((0, 8), (1, 16)), jnp.float32)
    gate_scale = jnp.clip(jnp.exp(jax.random.uniform(streams_of[7], (FF,), jnp.float32, math.log(0.5), math.log(2.0))), 0.5, 2.0)
    up_scale = jnp.clip(jnp.exp(jax.random.uniform(streams_of[8], (FF,), jnp.float32, math.log(0.5), math.log(2.0))), 0.5, 2.0)
    down_scale = jnp.clip(jnp.exp(jax.random.uniform(streams_of[9], (D,), jnp.float32, math.log(0.5), math.log(2.0))), 0.5, 2.0)
    mix_value = gaussian(streams_of[10], (D, D), D ** -0.5, 0.125, ((0, 16), (1, 8)), jnp.float32)
    mix_gate = gaussian(streams_of[11], (D, D), D ** -0.5, 0.125, ((0, 16), (1, 8)), jnp.float32)
    value_scale = jnp.clip(jnp.exp(jax.random.uniform(streams_of[12], (D,), jnp.float32, math.log(0.5), math.log(2.0))), 0.5, 2.0)
    gating_scale = jnp.clip(jnp.exp(jax.random.uniform(streams_of[13], (D,), jnp.float32, math.log(0.5), math.log(2.0))), 0.5, 2.0)
    mix_taps = draw_mix_taps(jax.random.fold_in(streams_of[18], 71), 0)
    mix_gain = jnp.clip(1.0 + 0.18 * jax.random.normal(streams_of[15], (D,), jnp.float32), 0.1, 1.9)
    mix_out = gaussian(streams_of[16], (D, D), D ** -0.5, 0.125, ((0, 8), (1, 16)), jnp.float32)
    out_scale = jnp.clip(jnp.exp(jax.random.uniform(streams_of[17], (D,), jnp.float32, math.log(0.5), math.log(2.0))), 0.5, 2.0)
    return dict(residual=residual, gain_first=gain_first, gain_mixer=gain_mixer, gain_last=gain_last, hidden_gate=hidden_gate, hidden_up=hidden_up, hidden_down=hidden_down, gate_scale=gate_scale, up_scale=up_scale, down_scale=down_scale, mix_value=mix_value, mix_gate=mix_gate, value_scale=value_scale, gating_scale=gating_scale, mix_taps=mix_taps, mix_gain=mix_gain, mix_out=mix_out, out_scale=out_scale)


EPS = 1e-06

def normalize(stream, gain):
    values = stream.astype(jnp.float32)
    scaled = values * lax.rsqrt(lax.optimization_barrier(jnp.mean(values * values, axis=-1, keepdims=True)) + EPS) * gain
    return scaled.astype(jnp.bfloat16)

def block_sum(left, weight, scale):
    blocks = left.shape[1] // N_TP
    total = jnp.zeros((left.shape[0], weight.shape[1]), jnp.float32)
    for index in range(N_TP):
        piece = jnp.dot(left[:, index * blocks:(index + 1) * blocks], weight[index * blocks:(index + 1) * blocks], preferred_element_type=jnp.float32) * scale
        total = total + lax.optimization_barrier(piece.astype(jnp.bfloat16)).astype(jnp.float32)
    return total

def inner_half(stream, gain, gate_w, up_w, down_w, gate_scale, up_scale, down_scale):
    normed = normalize(stream, gain)
    gate = jnp.dot(normed, gate_w, preferred_element_type=jnp.float32) * gate_scale
    upward = jnp.dot(normed, up_w, preferred_element_type=jnp.float32) * up_scale
    hidden = (jax.nn.silu(gate) * upward).astype(jnp.bfloat16)
    return block_sum(hidden, down_w, down_scale)

def mixer(stream, gain, value_w, gate_w, value_scale, gating_scale, taps, mix_gain, out_w, out_scale):
    normed = normalize(stream, gain)
    value = jnp.dot(normed, value_w, preferred_element_type=jnp.float32) * value_scale
    gating = jnp.dot(normed, gate_w, preferred_element_type=jnp.float32) * gating_scale
    glu = lax.optimization_barrier((value * jax.nn.sigmoid(gating)).astype(jnp.bfloat16)).astype(jnp.float32)
    length = glu.shape[0]
    span = taps.shape[0]
    padded = jnp.pad(glu, ((span - 1, 0), (0, 0)))
    wave = jnp.zeros_like(glu)
    for offset in range(span):
        wave = wave + taps[offset] * padded[span - 1 - offset:span - 1 - offset + length]
    acted = jax.nn.silu(wave * lax.rsqrt(lax.optimization_barrier(jnp.mean(wave * wave, axis=-1, keepdims=True)) + EPS) * mix_gain).astype(jnp.bfloat16)
    return block_sum(acted, out_w, out_scale)

def reference(residual, gain_first, gain_mixer, gain_last, hidden_gate, hidden_up, hidden_down, gate_scale, up_scale, down_scale, mix_value, mix_gate, value_scale, gating_scale, mix_taps, mix_gain, mix_out, out_scale):
    gate_w = hidden_gate.astype(jnp.bfloat16)
    up_w = hidden_up.astype(jnp.bfloat16)
    down_w = hidden_down.astype(jnp.bfloat16)
    value_w = mix_value.astype(jnp.bfloat16)
    mgate_w = mix_gate.astype(jnp.bfloat16)
    out_w = mix_out.astype(jnp.bfloat16)

    def one_sequence(stream):
        first = (stream.astype(jnp.float32) + 0.5 * inner_half(stream, gain_first, gate_w, up_w, down_w, gate_scale, up_scale, down_scale)).astype(jnp.bfloat16)
        second = (first.astype(jnp.float32) + mixer(first, gain_mixer, value_w, mgate_w, value_scale, gating_scale, mix_taps, mix_gain, out_w, out_scale)).astype(jnp.bfloat16)
        return (second.astype(jnp.float32) + 0.5 * inner_half(second, gain_last, gate_w, up_w, down_w, gate_scale, up_scale, down_scale)).astype(jnp.bfloat16)
    return lax.map(one_sequence, residual)
```

```python
import functools

import jax
import jax.numpy as jnp
from jax import lax
from jax.experimental import pallas as pl
from jax.experimental.pallas import tpu as pltpu
from jax.sharding import Mesh
from jax.sharding import PartitionSpec as P

EPS = 1e-06
BF = jnp.bfloat16
F32 = jnp.float32

REL = (0, 3, 1, 2)
VMEM = pl.BlockSpec(memory_space=pltpu.VMEM)
SMEM = pl.BlockSpec(memory_space=pltpu.SMEM)


def ring(n, k):
    return [(i, (i + k) % n) for i in range(n)]


def along_y(v, k):
    return lax.ppermute(v, "y", ring(4, k))


def along_z(v, k):
    return lax.ppermute(v, ("rep", "z"), ring(8, k))


def other_core(v):
    return lax.ppermute(v, "core", [(0, 1), (1, 0)])


def spread(v, axis):
    return lax.all_to_all(jnp.broadcast_to(v, (4, *v.shape)), axis, 0, 0, tiled=True)


def onward(stack, move):
    before, after = move(stack, 1), move(stack, -1)
    return stack, before, after, move(before[:2], 1), move(after[2:], -1)


def y_then_z(shard):
    return onward(spread(shard, "y"), along_z)


def z_then_y(shard):
    before, after = along_z(shard, 1), along_z(shard, -1)
    far = along_z(before, 1)
    return onward(jnp.stack([shard, before, after, far]), along_y)


def dot(a, b):
    return jnp.dot(a, b, preferred_element_type=F32)


def call(kernel, outs, scratch, flops, *args, limit=30):
    return pl.pallas_call(
        kernel,
        out_shape=outs,
        in_specs=[SMEM] + [VMEM] * (len(args) - 1),
        out_specs=jax.tree.map(lambda _: VMEM, outs),
        scratch_shapes=scratch,
        compiler_params=pltpu.CompilerParams(vmem_limit_bytes=limit * 2**20),
        cost_estimate=pl.CostEstimate(flops=flops, bytes_accessed=2**22, transcendentals=0),
    )(*args)


def pack_kernel(idx, gate, up, down, value, mgate, out, h1, h2, mx):
    h1[:, :768] = gate[...].astype(BF)
    h2[:, :768] = up[...].astype(BF)
    for j in range(3):
        cols = pl.ds(768 + j * 128, 128)
        h1[:, cols] = down[j * 128 : (j + 1) * 128].astype(BF)
        h2[:, cols] = down[(j + 3) * 128 : (j + 4) * 128].astype(BF)
    mx[:, :256] = value[...].astype(BF)
    mx[:, 256:512] = mgate[...].astype(BF)
    mx[:, 512:640] = out[:128].astype(BF)
    mx[:, 640:] = out[128:].astype(BF)


def pack(idx, *weights):
    shapes = [(128, 1152), (128, 1152), (128, 768)]
    outs = [jax.ShapeDtypeStruct(s, BF) for s in shapes]
    return call(pack_kernel, outs, [], 10**6, idx, *weights)


def normalize(idx, mine, theirs, gain, normed):
    core = idx[2]

    def rows_of(m, carry):
        rows = pl.ds(pl.multiple_of(m * 128, 128), 128)
        blocks = [r[x, rows].astype(F32) for r in (mine, theirs) for x in range(4)]
        total = sum(jnp.sum(b * b, axis=1, keepdims=True) for b in blocks)
        inverse = lax.rsqrt(total / 2048 + EPS)
        for k, b in enumerate(blocks):
            c = core if k < 4 else 1 - core
            cols = pl.ds(pl.multiple_of((2 * (k % 4) + c) * 256, 256), 256)
            normed[rows, cols] = (b * inverse * gain[:, cols]).astype(BF)
        return carry

    lax.fori_loop(0, 3, rows_of, 0)


def at(place, k):
    return lax.rem(place + REL[k], 4)


def z_chunks(idx, stacks):
    for k in range(3):
        yield at(idx[0], k) * 512, stacks[k], 4
    yield at(idx[0], 3) * 512, stacks[3], 2
    yield at(idx[0], 3) * 512 + 256, stacks[4], 2


def y_chunks(idx, stacks):
    for k in range(3):
        yield (0, 1, 2, 3), at(idx[1], k), stacks[k]
    yield (0, 1), at(idx[1], 3), stacks[3]
    yield (2, 3), at(idx[1], 3), stacks[4]


def ffn_kernel(idx, mine, theirs, gain, gate_scale, up_scale, down_scale, *refs):
    first, second = refs[:5], refs[5:10]
    keep, send, normed, hidden, acc = refs[10:]
    normalize(idx, mine, theirs, gain, normed)
    rank, core = idx[3], idx[2]

    def columns(n, carry):
        cols = pl.ds(pl.multiple_of(n * 256, 256), 256)
        gate = jnp.zeros((384, 256), F32)
        for start, ref, depth in z_chunks(idx, first):
            x = normed[:, pl.ds(pl.multiple_of(start, 256), depth * 128)]
            gate += dot(x, ref[:, :, cols].reshape(depth * 128, 256))
        up = jnp.zeros((384, 256), F32)
        for zs, y, ref in y_chunks(idx, second):
            x = jnp.concatenate(
                [normed[:, pl.ds(pl.multiple_of((at(idx[0], z) * 4 + y) * 128, 128), 128)] for z in zs],
                axis=1,
            )
            up += dot(x, ref[:, :, cols].reshape(len(zs) * 128, 256))
        scales = pl.ds(pl.multiple_of(rank * 768 + n * 256, 256), 256)
        gate = gate * gate_scale[:, scales]
        up = up * up_scale[:, scales]
        hidden[:, cols] = (gate / (1 + jnp.exp(-gate)) * up).astype(BF)
        return carry

    lax.fori_loop(0, 3, columns, 0)

    left = hidden[:, :384]
    for start, ref, depth in z_chunks(idx, first):
        for j in range(0, depth, 2):
            pair = [
                jnp.concatenate([ref[i, :, 768 + b * 128 : 896 + b * 128] for b in range(3)], axis=0)
                for i in (j, j + 1)
            ]
            cols = pl.ds(pl.multiple_of(start + j * 128, 256), 256)
            acc[:, cols] = dot(left, jnp.concatenate(pair, axis=1))
    left = hidden[:, 384:]
    for zs, y, ref in y_chunks(idx, second):
        for i, z in enumerate(zs):
            piece = jnp.concatenate([ref[i, :, 768 + b * 128 : 896 + b * 128] for b in range(3)], axis=0)
            cols = pl.ds(pl.multiple_of((at(idx[0], z) * 4 + y) * 128, 128), 128)
            acc[:, cols] += dot(left, piece)
    hand_out(core, acc, down_scale, keep, send)


def hand_out(core, acc, scale, keep, send):
    for x in range(4):
        cols = pl.ds(pl.multiple_of((2 * x + core) * 256, 256), 256)
        keep[x] = acc[:, cols] * scale[:, cols]
        cols = pl.ds(pl.multiple_of((2 * x + 1 - core) * 256, 256), 256)
        send[x] = (acc[:, cols] * scale[:, cols]).astype(BF)


TERMS = [jax.ShapeDtypeStruct((4, 384, 256), F32), jax.ShapeDtypeStruct((4, 384, 256), BF)]


def ffn(*args):
    scratch = [
        pltpu.VMEM((384, 2048), BF),
        pltpu.VMEM((384, 768), BF),
        pltpu.VMEM((384, 2048), F32),
    ]
    return call(ffn_kernel, TERMS, scratch, 2 * 384 * 2048 * 768 * 3, *args)


def mix_kernel(idx, mine, theirs, gain, value_scale, gating_scale, *refs):
    stacks = refs[:5]
    glu, normed = refs[5:]
    normalize(idx, mine, theirs, gain, normed)
    both = jnp.zeros((384, 512), F32)
    for start, ref, depth in z_chunks(idx, stacks):
        x = normed[:, pl.ds(pl.multiple_of(start, 256), depth * 128)]
        both += dot(x, ref[:, :, :512].reshape(depth * 128, 512))
    scales = pl.ds(pl.multiple_of(idx[3] * 256, 256), 256)
    value = both[:, :256] * value_scale[:, scales]
    gating = both[:, 256:] * gating_scale[:, scales]
    glu[...] = (value / (1 + jnp.exp(-gating))).astype(BF)


def mix(*args):
    out = jax.ShapeDtypeStruct((384, 256), BF)
    scratch = [pltpu.VMEM((384, 2048), BF)]
    return call(mix_kernel, out, scratch, 2 * 384 * 2048 * 512, *args)


def out_kernel(idx, acted, scale, *refs):
    stacks = refs[:5]
    keep, send, acc = refs[5:]
    left = acted[...]
    for start, ref, depth in z_chunks(idx, stacks):
        for j in range(0, depth, 2):
            pair = [
                jnp.concatenate([ref[i, :, 512:640], ref[i, :, 640:768]], axis=0) for i in (j, j + 1)
            ]
            cols = pl.ds(pl.multiple_of(start + j * 128, 256), 256)
            acc[:, cols] = dot(left, jnp.concatenate(pair, axis=1))
    hand_out(idx[2], acc, scale, keep, send)


def out_product(*args):
    scratch = [pltpu.VMEM((384, 2048), F32)]
    return call(out_kernel, TERMS, scratch, 2 * 384 * 2048 * 256, *args)


def whole_rows(stream):
    mine = spread(stream, "x")
    return mine, other_core(mine)


def summed(keep, send):
    chip = (keep + other_core(send).astype(F32)).astype(BF)
    return jnp.sum(lax.all_to_all(chip, "x", 0, 0, tiled=True).astype(F32), axis=0)


def on_device(
    residual,
    gain_first,
    gain_mixer,
    gain_last,
    hidden_gate,
    hidden_up,
    hidden_down,
    gate_scale,
    up_scale,
    down_scale,
    mix_value,
    mix_gate,
    value_scale,
    gating_scale,
    mix_taps,
    mix_gain,
    mix_out,
    out_scale,
):
    core = lax.axis_index("core")
    rank = 2 * lax.axis_index("x") + core
    idx = jnp.stack([lax.axis_index("z"), lax.axis_index("y"), core, rank]).astype(jnp.int32)
    row = lambda v: v.reshape(1, -1)
    h1, h2, mx = pack(idx, hidden_gate, hidden_up, hidden_down, mix_value, mix_gate, mix_out)
    stream = residual[0]
    wide = whole_rows(stream)
    second_half = z_then_y(h2)
    first_half = y_then_z(h1)
    mixing = y_then_z(mx)

    def half_step(wide, gain):
        scales = (row(gain), row(gate_scale), row(up_scale), row(down_scale))
        return summed(*ffn(idx, *wide, *scales, *first_half, *second_half))

    first = (stream.astype(F32) + 0.5 * half_step(wide, gain_first)).astype(BF)
    glu = mix(
        idx, *whole_rows(first), row(gain_mixer), row(value_scale), row(gating_scale), *mixing
    ).astype(F32)
    gain_cols = lax.dynamic_slice_in_dim(mix_gain, rank * 256, 256)
    tap_cols = lax.dynamic_slice_in_dim(mix_taps, rank * 256, 256, 1)
    padded = jnp.pad(glu, ((30, 0), (0, 0)))
    wave = jnp.zeros_like(glu)
    for offset in range(31):
        wave = wave + tap_cols[offset] * padded[30 - offset : 414 - offset]
    total_sq = lax.psum(jnp.sum(wave * wave, axis=1), ("x", "core"))
    inverse = lax.rsqrt(total_sq / 2048 + EPS)
    acted = jax.nn.silu(wave * inverse[:, None] * gain_cols).astype(BF)
    second = (first.astype(F32) + summed(*out_product(idx, acted, row(out_scale), *mixing))).astype(BF)
    updated = second.astype(F32) + 0.5 * half_step(whole_rows(second), gain_last)
    return updated.astype(BF)[None]


def solution(mesh):
    fine = Mesh(mesh.devices.reshape(2, 4, 4, 4, 2), ("rep", "z", "y", "x", "core"))
    fs, tp = ("z", "y"), ("x", "core")
    rows, cols, same = P(fs, tp), P(tp, fs), P()
    stream = P(("rep", "z", "y"), None, tp)
    in_specs = (stream, same, same, same, rows, rows, cols, same, same, same)
    in_specs += (rows, rows, same, same, same, same, cols, same)
    return jax.shard_map(
        on_device, mesh=fine, in_specs=in_specs, out_specs=stream, check_vma=False
    )
```

```python
import jax
import jax.numpy as jnp
from jax import lax
from jax.experimental import pallas as pl
from jax.experimental.pallas import tpu as pltpu
from jax.sharding import Mesh
from jax.sharding import PartitionSpec as P


EPS = 1e-06
BF = jnp.bfloat16
F32 = jnp.float32

REL = (0, 3, 1, 2)
VMEM = pl.BlockSpec(memory_space=pltpu.VMEM)
SMEM = pl.BlockSpec(memory_space=pltpu.SMEM)


def ring(n, k):
    return [(i, (i + k) % n) for i in range(n)]


def along_y(v, k):
    return lax.ppermute(v, "y", ring(4, k))


def along_z(v, k):
    return lax.ppermute(v, ("rep", "z"), ring(8, k))


def other_core(v):
    return lax.ppermute(v, "core", [(0, 1), (1, 0)])


def spread(v, axis):
    return lax.all_to_all(jnp.broadcast_to(v, (4, *v.shape)), axis, 0, 0, tiled=True)


def onward(stack, move):
    before, after = move(stack, 1), move(stack, -1)
    return stack, before, after, move(before[:2], 1), move(after[2:], -1)


def y_then_z(shard):
    return onward(spread(shard, "y"), along_z)


def z_then_y(shard):
    before, after = along_z(shard, 1), along_z(shard, -1)
    far = along_z(before, 1)
    return onward(jnp.stack([shard, before, after, far]), along_y)


def dot(a, b):
    return jnp.dot(a, b, preferred_element_type=F32)


def call(kernel, outs, scratch, flops, *args, limit=30):
    return pl.pallas_call(
        kernel,
        out_shape=outs,
        in_specs=[SMEM] + [VMEM] * (len(args) - 1),
        out_specs=jax.tree.map(lambda _: VMEM, outs),
        scratch_shapes=scratch,
        compiler_params=pltpu.CompilerParams(vmem_limit_bytes=limit * 2**20),
        cost_estimate=pl.CostEstimate(flops=flops, bytes_accessed=2**22, transcendentals=0),
    )(*args)


def pack_kernel(idx, gate, up, down, value, mgate, out, h1, h2, mx, *scratch):
    held, sems = scratch[:6], scratch[6]
    moves = [
        pltpu.make_async_copy(src, dst, sems.at[k])
        for k, (src, dst) in enumerate(zip((up, down, gate, value, mgate, out), held))
    ]
    for move in moves:
        move.start()
    up, down, gate, value, mgate, out = held
    moves[0].wait()
    h2[:, :768] = up[...].astype(BF)
    moves[1].wait()
    for j in range(3):
        cols = pl.ds(768 + j * 128, 128)
        h1[:, cols] = down[j * 128 : (j + 1) * 128].astype(BF)
        h2[:, cols] = down[(j + 3) * 128 : (j + 4) * 128].astype(BF)
    moves[2].wait()
    h1[:, :768] = gate[...].astype(BF)
    moves[3].wait()
    mx[:, :256] = value[...].astype(BF)
    moves[4].wait()
    mx[:, 256:512] = mgate[...].astype(BF)
    moves[5].wait()
    mx[:, 512:640] = out[:128].astype(BF)
    mx[:, 640:] = out[128:].astype(BF)


def pack(idx, *weights):
    shapes = [(128, 1152), (128, 1152), (128, 768)]
    outs = [jax.ShapeDtypeStruct(s, BF) for s in shapes]
    held = [(128, 768), (768, 128), (128, 768), (128, 256), (128, 256), (256, 128)]
    return pl.pallas_call(
        pack_kernel,
        out_shape=outs,
        in_specs=[SMEM] + [pl.BlockSpec(memory_space=pltpu.HBM)] * 6,
        out_specs=[VMEM] * 3,
        scratch_shapes=[pltpu.VMEM(s, F32) for s in held] + [pltpu.SemaphoreType.DMA((6,))],
        compiler_params=pltpu.CompilerParams(vmem_limit_bytes=8 * 2**20),
        cost_estimate=pl.CostEstimate(flops=10**6, bytes_accessed=2**21, transcendentals=0),
    )(idx, *weights)


def normalize(idx, mine, theirs, gain, normed):
    core = idx[2]

    def rows_of(m, carry):
        rows = pl.ds(pl.multiple_of(m * 128, 128), 128)
        blocks = [r[x, rows].astype(F32) for r in (mine, theirs) for x in range(4)]
        total = sum(jnp.sum(b * b, axis=1, keepdims=True) for b in blocks)
        inverse = lax.rsqrt(total / 2048 + EPS)
        for k, b in enumerate(blocks):
            c = core if k < 4 else 1 - core
            cols = pl.ds(pl.multiple_of((2 * (k % 4) + c) * 256, 256), 256)
            normed[rows, cols] = (b * inverse * gain[:, cols]).astype(BF)
        return carry

    lax.fori_loop(0, 3, rows_of, 0)


def at(place, k):
    return lax.rem(place + REL[k], 4)


def z_chunks(idx, stacks):
    for k in range(3):
        yield at(idx[0], k) * 512, stacks[k], 4
    yield at(idx[0], 3) * 512, stacks[3], 2
    yield at(idx[0], 3) * 512 + 256, stacks[4], 2


def y_chunks(idx, stacks):
    for k in range(3):
        yield (0, 1, 2, 3), at(idx[1], k), stacks[k]
    yield (0, 1), at(idx[1], 3), stacks[3]
    yield (2, 3), at(idx[1], 3), stacks[4]


def ffn_kernel(idx, mine, theirs, gain, gate_scale, up_scale, down_scale, *refs):
    first, second = refs[:5], refs[5:10]
    keep, send, normed, hidden, acc = refs[10:]
    normalize(idx, mine, theirs, gain, normed)
    rank, core = idx[3], idx[2]

    def columns(n, carry):
        cols = pl.ds(pl.multiple_of(n * 256, 256), 256)
        gate = jnp.zeros((384, 256), F32)
        for start, ref, depth in z_chunks(idx, first):
            x = normed[:, pl.ds(pl.multiple_of(start, 256), depth * 128)]
            gate += dot(x, ref[:, :, cols].reshape(depth * 128, 256))
        up = jnp.zeros((384, 256), F32)
        for zs, y, ref in y_chunks(idx, second):
            x = jnp.concatenate(
                [normed[:, pl.ds(pl.multiple_of((at(idx[0], z) * 4 + y) * 128, 128), 128)] for z in zs],
                axis=1,
            )
            up += dot(x, ref[:, :, cols].reshape(len(zs) * 128, 256))
        scales = pl.ds(pl.multiple_of(rank * 768 + n * 256, 256), 256)
        gate = gate * gate_scale[:, scales]
        up = up * up_scale[:, scales]
        hidden[:, cols] = (gate / (1 + jnp.exp(-gate)) * up).astype(BF)
        return carry

    lax.fori_loop(0, 3, columns, 0)

    left = hidden[:, :384]
    for start, ref, depth in z_chunks(idx, first):
        for j in range(0, depth, 2):
            pair = [
                jnp.concatenate([ref[i, :, 768 + b * 128 : 896 + b * 128] for b in range(3)], axis=0)
                for i in (j, j + 1)
            ]
            cols = pl.ds(pl.multiple_of(start + j * 128, 256), 256)
            acc[:, cols] = dot(left, jnp.concatenate(pair, axis=1))
    left = hidden[:, 384:]
    for zs, y, ref in y_chunks(idx, second):
        for i, z in enumerate(zs):
            piece = jnp.concatenate([ref[i, :, 768 + b * 128 : 896 + b * 128] for b in range(3)], axis=0)
            cols = pl.ds(pl.multiple_of((at(idx[0], z) * 4 + y) * 128, 128), 128)
            acc[:, cols] += dot(left, piece)
    hand_out(core, acc, down_scale, keep, send)


def hand_out(core, acc, scale, keep, send):
    for x in range(4):
        cols = pl.ds(pl.multiple_of((2 * x + core) * 256, 256), 256)
        keep[x] = acc[:, cols] * scale[:, cols]
        cols = pl.ds(pl.multiple_of((2 * x + 1 - core) * 256, 256), 256)
        send[x] = (acc[:, cols] * scale[:, cols]).astype(BF)


TERMS = [jax.ShapeDtypeStruct((4, 384, 256), F32), jax.ShapeDtypeStruct((4, 384, 256), BF)]


def ffn(*args):
    scratch = [
        pltpu.VMEM((384, 2048), BF),
        pltpu.VMEM((384, 768), BF),
        pltpu.VMEM((384, 2048), F32),
    ]
    return call(ffn_kernel, TERMS, scratch, 2 * 384 * 2048 * 768 * 3, *args)


def mix_kernel(idx, mine, theirs, gain, value_scale, gating_scale, *refs):
    stacks = refs[:5]
    glu, normed = refs[5:]
    normalize(idx, mine, theirs, gain, normed)
    both = jnp.zeros((384, 512), F32)
    for start, ref, depth in z_chunks(idx, stacks):
        x = normed[:, pl.ds(pl.multiple_of(start, 256), depth * 128)]
        both += dot(x, ref[:, :, :512].reshape(depth * 128, 512))
    scales = pl.ds(pl.multiple_of(idx[3] * 256, 256), 256)
    value = both[:, :256] * value_scale[:, scales]
    gating = both[:, 256:] * gating_scale[:, scales]
    glu[...] = (value / (1 + jnp.exp(-gating))).astype(BF)


def mix(*args):
    out = jax.ShapeDtypeStruct((384, 256), BF)
    scratch = [pltpu.VMEM((384, 2048), BF)]
    return call(mix_kernel, out, scratch, 2 * 384 * 2048 * 512, *args)


def out_kernel(idx, acted, scale, *refs):
    stacks = refs[:5]
    keep, send, acc = refs[5:]
    left = acted[...]
    for start, ref, depth in z_chunks(idx, stacks):
        for j in range(0, depth, 2):
            pair = [
                jnp.concatenate([ref[i, :, 512:640], ref[i, :, 640:768]], axis=0) for i in (j, j + 1)
            ]
            cols = pl.ds(pl.multiple_of(start + j * 128, 256), 256)
            acc[:, cols] = dot(left, jnp.concatenate(pair, axis=1))
    hand_out(idx[2], acc, scale, keep, send)


def out_product(*args):
    scratch = [pltpu.VMEM((384, 2048), F32)]
    return call(out_kernel, TERMS, scratch, 2 * 384 * 2048 * 256, *args)


def whole_rows(stream):
    mine = lax.all_gather(stream, "x", axis=0)
    return mine, other_core(mine)


def summed(keep, send):
    chip = (keep + other_core(send).astype(F32)).astype(BF)
    return jnp.sum(lax.all_to_all(chip, "x", 0, 0, tiled=True).astype(F32), axis=0)


def on_device(
    residual,
    gain_first,
    gain_mixer,
    gain_last,
    hidden_gate,
    hidden_up,
    hidden_down,
    gate_scale,
    up_scale,
    down_scale,
    mix_value,
    mix_gate,
    value_scale,
    gating_scale,
    mix_taps,
    mix_gain,
    mix_out,
    out_scale,
):
    core = lax.axis_index("core")
    rank = 2 * lax.axis_index("x") + core
    idx = jnp.stack([lax.axis_index("z"), lax.axis_index("y"), core, rank]).astype(jnp.int32)
    row = lambda v: v.reshape(1, -1)
    h1, h2, mx = pack(idx, hidden_gate, hidden_up, hidden_down, mix_value, mix_gate, mix_out)
    stream = residual[0]
    wide = whole_rows(stream)
    second_half = z_then_y(h2)
    first_half = y_then_z(h1)
    mx, _ = lax.optimization_barrier((mx, second_half[0]))
    mixing = spread(mx, "y")
    ready, mixing = lax.optimization_barrier((idx, mixing))
    before, after = along_z(mixing, 1), along_z(mixing, -1)
    far = along_z(before[:2], 1), along_z(after[2:], -1)
    mixing = (mixing, before, after, *far)

    def half_step(wide, gain, idx):
        scales = (row(gain), row(gate_scale), row(up_scale), row(down_scale))
        return summed(*ffn(idx, *wide, *scales, *first_half, *second_half))

    first = half_step(wide, gain_first, ready)
    first = (stream.astype(F32) + 0.5 * first).astype(BF)
    glu = mix(
        idx, *whole_rows(first), row(gain_mixer), row(value_scale), row(gating_scale), *mixing
    ).astype(F32)
    gain_cols = lax.dynamic_slice_in_dim(mix_gain, rank * 256, 256)
    tap_cols = lax.dynamic_slice_in_dim(mix_taps, rank * 256, 256, 1)
    padded = jnp.pad(glu, ((30, 0), (0, 0)))
    wave = jnp.zeros_like(glu)
    for offset in range(31):
        wave = wave + tap_cols[offset] * padded[30 - offset : 414 - offset]
    squares = jnp.broadcast_to(jnp.sum(wave * wave, axis=1), (8, 384))
    total_sq = jnp.sum(lax.all_to_all(squares, ("x", "core"), 0, 0, tiled=True), axis=0)
    inverse = lax.rsqrt(total_sq / 2048 + EPS)
    acted = jax.nn.silu(wave * inverse[:, None] * gain_cols).astype(BF)
    second = (first.astype(F32) + summed(*out_product(idx, acted, row(out_scale), *mixing))).astype(BF)
    updated = second.astype(F32) + 0.5 * half_step(whole_rows(second), gain_last, idx)
    return updated.astype(BF)[None]


def solution(mesh):
    fine = Mesh(mesh.devices.reshape(2, 4, 4, 4, 2), ("rep", "z", "y", "x", "core"))
    fs, tp = ("z", "y"), ("x", "core")
    rows, cols, same = P(fs, tp), P(tp, fs), P()
    stream = P(("rep", "z", "y"), None, tp)
    in_specs = (stream, same, same, same, rows, rows, cols, same, same, same)
    in_specs += (rows, rows, same, same, same, same, cols, same)
    return jax.shard_map(on_device, mesh=fine, in_specs=in_specs, out_specs=stream, check_vma=False)
```

```python
import functools

import jax
import jax.numpy as jnp
from jax import lax
from jax.experimental import pallas as pl
from jax.experimental.pallas import tpu as pltpu
from jax.sharding import Mesh
from jax.sharding import PartitionSpec as P


EPS = 1e-06
BF = jnp.bfloat16
F32 = jnp.float32

REL = (0, 3, 1, 2)
PACK_LIMIT = 67043328 - 832 * 1024
VMEM = pl.BlockSpec(memory_space=pltpu.VMEM)


def ring(n, k):
    return [(i, (i + k) % n) for i in range(n)]


def along_y(v, k):
    return lax.ppermute(v, "y", ring(4, k))


def along_z(v, k):
    return lax.ppermute(v, ("rep", "z"), ring(8, k))


def other_core(v):
    return lax.ppermute(v, "core", [(0, 1), (1, 0)])


def spread(v, axis):
    return lax.all_to_all(jnp.broadcast_to(v, (4, *v.shape)), axis, 0, 0, tiled=True)


def onward(stack, move):
    before, after = move(stack, 1), move(stack, -1)
    return stack, before, after, move(before[:2], 1), move(after[2:], -1)


def every_z(shard):
    before, after = along_z(shard, 1), along_z(shard, -1)
    return jnp.stack([shard, before, after, along_z(before, 1)])


def dot(a, b):
    return jnp.dot(a, b, preferred_element_type=F32)


def call(kernel, outs, scratch, flops, *args, limit=16):
    return pl.pallas_call(
        kernel,
        out_shape=outs,
        in_specs=[VMEM] * len(args),
        out_specs=jax.tree.map(lambda _: VMEM, outs),
        scratch_shapes=scratch,
        compiler_params=pltpu.CompilerParams(vmem_limit_bytes=limit * 2**20),
        cost_estimate=pl.CostEstimate(flops=flops, bytes_accessed=2**22, transcendentals=0),
    )(*args)


def pack_kernel(up, gate, down, value, mgate, out, second, first, mx, *scratch):
    held, sems = scratch[:6], scratch[6]
    moves = [
        pltpu.make_async_copy(src, dst, sems.at[k])
        for k, (src, dst) in enumerate(zip((up, gate, down, value, mgate, out), held))
    ]
    for move in moves:
        move.start()
    up, gate, down, value, mgate, out = held
    moves[0].wait()
    second[:, 384:] = up[...].astype(BF)
    moves[1].wait()
    first[:, :384] = gate[:, :384].astype(BF)
    second[:, :384] = gate[:, 384:].astype(BF)
    moves[2].wait()
    for j in range(6):
        first[:, 384 + j * 128 : 512 + j * 128] = down[j * 128 : (j + 1) * 128].astype(BF)
    moves[3].wait()
    mx[:, :256] = value[...].astype(BF)
    moves[4].wait()
    mx[:, 256:512] = mgate[...].astype(BF)
    moves[5].wait()
    mx[:, 512:640] = out[:128].astype(BF)
    mx[:, 640:] = out[128:].astype(BF)


def pack(*weights):
    outs = [jax.ShapeDtypeStruct((128, n), BF) for n in (1152, 1152, 768)]
    held = [(128, 768), (128, 768), (768, 128), (128, 256), (128, 256), (256, 128)]
    return pl.pallas_call(
        pack_kernel,
        out_shape=outs,
        in_specs=[pl.BlockSpec(memory_space=pltpu.HBM)] * 6,
        out_specs=[VMEM] * 3,
        scratch_shapes=[pltpu.VMEM(s, F32) for s in held] + [pltpu.SemaphoreType.DMA((6,))],
        compiler_params=pltpu.CompilerParams(vmem_limit_bytes=PACK_LIMIT),
        cost_estimate=pl.CostEstimate(flops=10**6, bytes_accessed=2**21, transcendentals=0),
    )(*weights)


def here():
    core, x = lax.axis_index("core"), lax.axis_index("x")
    return lax.axis_index("z"), lax.axis_index("y"), core, 2 * x + core, x


def at(place, k):
    return lax.rem(place + REL[k], 4)


def seen(place, me):
    d = lax.rem(place - me + 4, 4)
    return jnp.where(d == 0, 0, jnp.where(d == 3, 1, d + 1))


def scaled_rows(idx, turning, mine, theirs, gain, rows_out, inverse, turned=None):
    core, z, me = idx[2], idx[0], idx[4]

    def rows_of(m, carry):
        rows = pl.ds(pl.multiple_of(m * 128, 128), 128)
        total = jnp.zeros((128, 256), F32)
        for r in range(4):
            x = at(me, r) if turning else r
            for c, source in ((core, mine), (1 - core, theirs)):
                block = source[r, rows].astype(F32)
                total += block * block
                start = pl.multiple_of((2 * x + c) * 256, 256)
                block = (block * gain[:, pl.ds(start, 256)]).astype(BF)
                if turned is not None:
                    rows_out[rows, pl.ds(start, 256)] = block
                for h in range(2):
                    if turned is not None:
                        to, ref = (2 * c + h) * 512 + seen(x, z) * 128, turned
                    else:
                        to, ref = x * 512 + seen(2 * c + h, idx[1]) * 128, rows_out
                    to = pl.ds(pl.multiple_of(to, 128), 128)
                    ref[rows, to] = block[:, h * 128 : h * 128 + 128]
        total = jnp.sum(total, axis=1, keepdims=True)
        inverse[rows, :] = jnp.broadcast_to(lax.rsqrt(total / 2048 + EPS), (128, 128))
        return carry

    lax.fori_loop(0, 3, rows_of, 0)


def chunks(place, stacks):
    for k in range(3):
        yield at(place, k) * 512, stacks[k], 4
    yield at(place, 3) * 512, stacks[3], 2
    yield at(place, 3) * 512 + 256, stacks[4], 2


def product_of(rows, place, stacks, cols, width):
    total = jnp.zeros((384, width), F32)
    for start, ref, depth in chunks(place, stacks):
        x = rows[:, pl.ds(pl.multiple_of(start, 256), depth * 128)]
        total += dot(x, ref[:, :, cols].reshape(depth * 128, width))
    return total


def up_kernel(turning, mine, theirs, gain, gate_scale, up_scale, *refs):
    idx = here()
    first, second = refs[:5], refs[5:10]
    hidden, rows, turned, inverse, raw = refs[10:]
    scaled_rows(idx, turning, mine, theirs, gain, rows, inverse, turned)
    raw[:, :384] = product_of(rows, idx[0], first, pl.ds(0, 384), 384)

    def columns(n, carry):
        cols = pl.ds(pl.multiple_of(n * 384, 128), 384)
        to = pl.ds(pl.multiple_of(n * 384 + 384, 128), 384)
        raw[:, to] = product_of(turned, idx[1], second, cols, 384)
        return carry

    lax.fori_loop(0, 3, columns, 0)

    def units(n, carry):
        cols = pl.ds(pl.multiple_of(n * 128, 128), 128)
        ups = pl.ds(pl.multiple_of(768 + n * 128, 128), 128)
        scales = pl.ds(pl.multiple_of(idx[3] * 768 + n * 128, 128), 128)
        gate = raw[:, cols] * inverse[...] * gate_scale[:, scales]
        up = raw[:, ups] * inverse[...] * up_scale[:, scales]
        hidden[:, cols] = (gate / (1 + jnp.exp(-gate)) * up).astype(BF)
        return carry

    lax.fori_loop(0, 6, units, 0)


def up_product(turning, *args):
    out = jax.ShapeDtypeStruct((384, 768), BF)
    scratch = [
        pltpu.VMEM((384, 2048), BF),
        pltpu.VMEM((384, 2048), BF),
        pltpu.VMEM((384, 128), F32),
        pltpu.VMEM((384, 1536), F32),
    ]
    return call(functools.partial(up_kernel, turning), out, scratch, 2 * 384 * 2048 * 768 * 2, *args)


def tall(piece, first, blocks):
    return jnp.concatenate([piece[:, first + b * 128 : first + b * 128 + 128] for b in range(blocks)], axis=0)


def hand_out(idx, left, pick, scale, keep, send):
    core = idx[2]
    for k in range(4):
        x = at(idx[0], k)
        pair = []
        for c in range(2):
            wide = jnp.concatenate([pick(k, 2 * c + i) for i in range(2)], axis=1)
            cols = pl.ds(pl.multiple_of(x * 512 + c * 256, 256), 256)
            pair.append(dot(left, wide) * scale[:, cols])
        r = seen(x, idx[4])
        keep[r] = jnp.where(core == 0, pair[0], pair[1])
        send[r] = jnp.where(core == 0, pair[1], pair[0]).astype(BF)


def down_kernel(hidden, scale, *refs):
    def pick(k, y):
        piece = refs[k][y] if k < 3 else refs[3 + y // 2][y % 2]
        return tall(piece, 384, 6)

    hand_out(here(), hidden[...], pick, scale, *refs[5:])


TERMS = [jax.ShapeDtypeStruct((4, 384, 256), F32), jax.ShapeDtypeStruct((4, 384, 256), BF)]


def down_product(*args):
    return call(down_kernel, TERMS, [], 2 * 384 * 2048 * 768, *args)


def mix_kernel(mine, theirs, gain, value_scale, gating_scale, taps, *refs):
    idx = here()
    stacks = refs[:5]
    wave, squares, rows, inverse, padded = refs[5:]
    scaled_rows(idx, True, mine, theirs, gain, rows, inverse)
    both = product_of(rows, idx[0], stacks, pl.ds(0, 512), 512)
    both *= inverse[:, :1]
    cols = pl.ds(pl.multiple_of(idx[3] * 256, 256), 256)
    value = both[:, :256] * value_scale[:, cols]
    gating = both[:, 256:] * gating_scale[:, cols]
    padded[:32] = jnp.zeros((32, 256), F32)
    padded[32:] = (value / (1 + jnp.exp(-gating))).astype(BF).astype(F32)

    def rows_of(m, carry):
        block = padded[pl.ds(pl.multiple_of(m * 64, 64), 96)]
        total = jnp.zeros((64, 256), F32)
        for shift in range(8):
            moved = block if shift == 0 else block[shift : shift + 88]
            for first in range(0, 33 if shift == 0 else 25, 8):
                tap = 32 - first - shift
                if tap <= 30:
                    total += taps[tap : tap + 1, cols] * moved[first : first + 64]
        wave[pl.ds(pl.multiple_of(m * 64, 64), 64)] = total
        return carry

    lax.fori_loop(0, 6, rows_of, 0)
    sums = jnp.sum(wave[...] * wave[...], axis=1, keepdims=True)
    flat = jnp.broadcast_to(sums, (384, 128)).T
    for k in range(8):
        squares[k] = flat[k : k + 1]


def mix(*args):
    outs = [jax.ShapeDtypeStruct((384, 256), F32), jax.ShapeDtypeStruct((8, 1, 384), F32)]
    scratch = [
        pltpu.VMEM((384, 2048), BF),
        pltpu.VMEM((384, 128), F32),
        pltpu.VMEM((416, 256), F32),
    ]
    return call(mix_kernel, outs, scratch, 2 * 384 * 2048 * 512, *args)


def out_kernel(wave, squares, gain, scale, *refs):
    idx = here()
    stacks, keep, send, far = refs[:5], *refs[5:]
    total = sum(squares[k] for k in range(8))
    inverse = lax.rsqrt(jnp.broadcast_to(total, (128, 384)).T / 2048 + EPS)
    halves = []
    for h in range(2):
        cols = pl.ds(pl.multiple_of(idx[3] * 256 + h * 128, 128), 128)
        a = wave[:, h * 128 : h * 128 + 128] * inverse * gain[:, cols]
        halves.append((a / (1 + jnp.exp(-a))).astype(BF))
    acted = jnp.concatenate(halves, axis=1)

    far[:2] = stacks[3][:, :, 512:]
    far[2:] = stacks[4][:, :, 512:]

    def pick(k, y):
        j = seen(y, idx[1])
        return tall(far[j], 0, 2) if k == 3 else tall(stacks[k][j], 512, 2)

    hand_out(idx, acted, pick, scale, keep, send)


def out_product(*args):
    scratch = [pltpu.VMEM((4, 128, 256), BF)]
    return call(out_kernel, TERMS, scratch, 2 * 384 * 2048 * 256, *args)


def across(v, k):
    return lax.ppermute(v, "x", ring(4, k))


def turned_rows(stream):
    mine = jnp.stack([stream, across(stream, 1), across(stream, -1), across(stream, 2)])
    return mine, other_core(mine)


def whole_rows(stream):
    mine = lax.all_gather(stream, "x", axis=0)
    return mine, other_core(mine)


def summed(keep, send):
    chip = keep + other_core(send).astype(F32)
    before, after, far = (chip[r].astype(BF) for r in (1, 2, 3))
    parts = across(before, -1), across(after, 1), across(far, 2)
    return chip[0] + sum(p.astype(F32) for p in parts)


def on_device(
    residual,
    gain_first,
    gain_mixer,
    gain_last,
    hidden_gate,
    hidden_up,
    hidden_down,
    gate_scale,
    up_scale,
    down_scale,
    mix_value,
    mix_gate,
    value_scale,
    gating_scale,
    mix_taps,
    mix_gain,
    mix_out,
    out_scale,
):
    row = lambda v: v.reshape(1, -1)
    second, first, mx = pack(hidden_up, hidden_gate, hidden_down, mix_value, mix_gate, mix_out)
    stream = residual[0]
    second = onward(every_z(second), along_y)
    first = onward(spread(first, "y"), along_z)
    mixing = [along_y(mx, k) for k in (1, -1, 2)]
    mixing = jnp.stack([mx, *mixing])
    before, after = along_z(mixing, 1), along_z(mixing, -1)
    far = along_z(before[:2], 1), along_z(after[2:], -1)
    mixing = (mixing, before, after, *far)
    wide = whole_rows(stream)

    def half_step(turning, wide, gain):
        scales = row(gain), row(gate_scale), row(up_scale)
        hidden = up_product(turning, *wide, *scales, *first, *second)
        terms = down_product(hidden, row(down_scale), *first)
        return summed(*terms)

    one = half_step(False, wide, gain_first)
    one = (stream.astype(F32) + 0.5 * one).astype(BF)
    wide = turned_rows(one)
    scales = (row(value_scale), row(gating_scale))
    wave, squares = mix(*wide, row(gain_mixer), *scales, mix_taps, *mixing)
    squares = lax.all_to_all(squares, ("x", "core"), 0, 0, tiled=True)
    terms = out_product(wave, squares, row(mix_gain), row(out_scale), *mixing)
    two = (one.astype(F32) + summed(*terms)).astype(BF)
    updated = two.astype(F32) + 0.5 * half_step(False, whole_rows(two), gain_last)
    return updated.astype(BF)[None]


def solution(mesh):
    fine = Mesh(mesh.devices.reshape(2, 4, 4, 4, 2), ("rep", "z", "y", "x", "core"))
    fs, tp = ("z", "y"), ("x", "core")
    rows, cols, same = P(fs, tp), P(tp, fs), P()
    stream = P(("rep", "z", "y"), None, tp)
    in_specs = (stream, same, same, same, rows, rows, cols, same, same, same)
    in_specs += (rows, rows, same, same, same, same, cols, same)
    return jax.shard_map(on_device, mesh=fine, in_specs=in_specs, out_specs=stream, check_vma=False)
```
